256 devices in a mesh: ep: 32 (over z, x), tp: 8 (over y, core).
Axes of the slice: x: 4, y: 4, z: 8, core: 2. Of those that a mesh axis runs over, the one named last changes fastest.
Arguments:
- tokens: bfloat16 [8192, 2048], P('ep'), may hold values from -6 to 6
- routes: int32 [8192, 2], P('ep'), may hold values from 0 to 31, all different within a row; in each aligned block of 256 rows (0 to 255, 256 to 511, ...) at most 32 rows name the same one
- router_matrix: bfloat16 [2048, 32], replicated, may hold values from -0.125 to 0.125
- cotangent: bfloat16 [8192, 2048], P('ep', 'tp'), may hold values from -3 to 3
- gate_proj: bfloat16 [32, 2048, 3584], P('ep', None, 'tp'), may hold values from -0.125 to 0.125
- up_proj: bfloat16 [32, 2048, 3584], P('ep', None, 'tp'), may hold values from -0.125 to 0.125
- down_proj: bfloat16 [32, 3584, 2048], P('ep', 'tp'), may hold values from -0.09375 to 0.09375
Outputs:
- token_grad: bfloat16 [8192, 2048], P('ep', 'tp')
- mixing_grad: float32 [8192, 2], P('ep')
- router_grad: float32 [2048, 32], P(('ep', 'tp'))
- gate_grad: bfloat16 [32, 2048, 3584], P('ep', None, 'tp')
- up_grad: bfloat16 [32, 2048, 3584], P('ep', None, 'tp')
- down_grad: bfloat16 [32, 3584, 2048], P('ep', 'tp')
The draws below stay inside these ranges and needn't reach their ends.
Inputs may be any that keep to these rules, and one draw needn't show every extreme that they name: `routes`: the two experts of a row differ. In each aligned block of 256 rows no expert is named by more than 32 rows, a bound that some block reaches; every expert is named somewhere.
All inputs are finite; a program needn't handle non-finite values.
Results may differ from the reference program's by a relative error of at most 0.019.
Values may be sent and summed in bfloat16 or wider, within the bound.
A program may use at most 128 MiB of HBM per device.

```python
import math
import jax
import jax.numpy as jnp
import numpy as np
from jax import lax

D = 2048
FF = 3584
TOP = 2
TOK_DEV = 256
EXPERTS = 32
TOKENS = 8192
CAP = 32
N_EP = 32
N_TP = 8


def steps_of(rng, extent, cuts, least, top_value):
    gain = 1.0
    for dim, shards_of in cuts:
        draws = jax.random.uniform(jax.random.fold_in(jax.random.fold_in(rng, 6), dim), (shards_of,), jnp.float32, least / len(cuts), top_value / len(cuts))
        gain = gain * jnp.repeat(jnp.exp(draws), extent[dim] // shards_of).reshape((-1,) + (1,) * (len(extent) - 1 - dim))
    return gain


def routed_block(own_key, own, number, rows, amount, top, most, slope):
    ranking = jax.random.permutation(own_key, amount)
    heavy_load, common = portions_of(amount, rows * top, most, slope, True), portions_of(amount, rows * top, most, slope, False)
    places = jnp.arange(amount)

    def named(tallies, rotation):
        used = int((tallies > 0).sum())
        fixed = max(1, used // 4)
        shifted = fixed + (places - fixed + rotation * (used - fixed)) % max(1, amount - fixed)
        return jnp.zeros((amount,), jnp.int32).at[ranking[jnp.where(places < fixed, places, shifted)]].set(jnp.asarray(tallies, jnp.int32))

    tallies = jnp.where(number % 4 == 0, named(heavy_load, number // 4), named(common, number - number // 4 - 1))
    mixed = jax.random.permutation(jax.random.fold_in(own, 3), amount)
    donor, sink = mixed[0:amount // 2 * 2:2], mixed[1:amount // 2 * 2:2]
    slack = jnp.minimum(tallies[donor] - 1, most - tallies[sink]) // 2
    slack = jnp.where((donor == ranking[0]) | (sink == ranking[0]) | (tallies[sink] == 0), 0, jnp.maximum(slack, 0))
    shifted = jax.random.randint(jax.random.fold_in(own, 4), (amount // 2,), 0, 1 << 20) % (slack + 1)
    tallies = tallies.at[donor].add(-shifted).at[sink].add(shifted)
    items = jnp.searchsorted(jnp.cumsum(tallies), jnp.arange(rows * top), side="right").astype(jnp.int32)
    table = items.reshape(top, rows).T
    table = table[jax.random.permutation(jax.random.fold_in(own, 1), rows)]
    rotation = jax.random.randint(jax.random.fold_in(own, 2), (rows, 1), 0, top)
    return jnp.take_along_axis(table, (jnp.arange(top)[None, :] + rotation) % top, axis=1)


def portions_of(number_of, total, limit, slope, full):
    weights = [(1 << 20) // math.isqrt(standing ** slope) + 1 for standing in range(1, number_of + 1)]
    largest = limit if full else min(limit, max(-(-total // number_of), total * weights[0] // sum(weights)))
    least = 1 if total - largest >= number_of - 1 else 0
    holding, surplus = [largest] + [least] * (number_of - 1), total - largest - least * (number_of - 1)
    while surplus > 0:
        movable = [i for i in range(1, number_of) if holding[i] < largest] or [i for i in range(1, number_of) if holding[i] < limit]
        whole, budget = sum([weights[i] for i in movable]), surplus
        for i in movable:
            addition = min(limit - holding[i], max(1, budget * weights[i] // whole), surplus)
            holding[i] = holding[i] + addition
            surplus = surplus - addition
    return np.array(holding)


def normal_values(own_key, dims, deviation, bound, split=(), kind=jnp.bfloat16):
    drawn = deviation * jax.random.normal(own_key, dims, jnp.float32)
    if split:
        drawn = drawn * steps_of(own_key, dims, split, -0.22, 0.18)
    return jnp.clip(drawn, -bound, bound).astype(kind)


def setup_inputs(seed: int = 0) -> dict:
    key_of = jax.random.split(jax.random.key(seed), 8)
    tokens = normal_values(key_of[0], (TOKENS, D), 1.0, 6.0, ((0, 32),))
    routes_keys = jax.random.split(jax.random.fold_in(key_of[1], 1), TOKENS // TOK_DEV)
    routes_turns = jax.random.permutation(jax.random.fold_in(key_of[1], 3), TOKENS // TOK_DEV)
    routes = jax.vmap(lambda own, number: routed_block(jax.random.fold_in(key_of[1], 2), own, number, TOK_DEV, EXPERTS, TOP, CAP, 2))(routes_keys, routes_turns).reshape((TOKENS, TOP))
    router_matrix = normal_values(key_of[2], (D, EXPERTS), D ** -0.5, 0.125)
    cotangent = normal_values(key_of[3], (TOKENS, D), 0.5, 3.0, ((0, 32), (1, 8)))
    gate_proj = normal_values(key_of[4], (EXPERTS, D, FF), D ** -0.5, 0.125, ((0, 32), (2, 8)))
    up_proj = normal_values(key_of[5], (EXPERTS, D, FF), D ** -0.5, 0.125, ((0, 32), (2, 8)))
    down_proj = normal_values(key_of[6], (EXPERTS, FF, D), FF ** -0.5, 0.09375, ((0, 32), (1, 8)))
    return {"tokens": tokens, "routes": routes, "router_matrix": router_matrix, "cotangent": cotangent, "gate_proj": gate_proj, "up_proj": up_proj, "down_proj": down_proj}


def slot_places(flat_routes, experts, capacity):
    onehot = (flat_routes[:, None] == jnp.arange(experts, dtype=jnp.int32)[None, :]).astype(jnp.int32)
    earlier = jnp.cumsum(onehot, axis=0) - onehot
    places = (flat_routes * capacity + lax.optimization_barrier(jnp.sum(earlier * onehot, axis=1))).astype(jnp.int32)
    entries = flat_routes.shape[0]
    filler = jnp.full((experts * capacity,), entries, jnp.int32).at[places].set(jnp.arange(entries, dtype=jnp.int32))
    return (places, filler)

def expert_pass(operands):
    token_rows, output_rows, mix_rows, w_gate, w_up, w_down = operands
    mix_value = mix_rows.astype(jnp.float32)
    gate_pre = jnp.dot(token_rows, w_gate, preferred_element_type=jnp.float32)
    up_pre = jnp.dot(token_rows, w_up, preferred_element_type=jnp.float32)
    gate_sig = jax.nn.sigmoid(gate_pre)
    active = gate_pre * gate_sig
    hidden = (active * up_pre).astype(jnp.bfloat16)
    back_hidden = jnp.dot(output_rows, w_down.T, preferred_element_type=jnp.float32)
    mix_part = lax.optimization_barrier(jnp.sum(hidden.astype(jnp.float32) * back_hidden, axis=1))
    scaled = mix_value[:, None] * back_hidden
    gate_back = (scaled * up_pre * gate_sig * (1.0 + gate_pre * (1.0 - gate_sig))).astype(jnp.bfloat16)
    up_back = (scaled * active).astype(jnp.bfloat16)
    out_scaled = (mix_value[:, None] * output_rows.astype(jnp.float32)).astype(jnp.bfloat16)
    gate_grad = jnp.dot(token_rows.T, gate_back, preferred_element_type=jnp.float32).astype(jnp.bfloat16)
    up_grad = jnp.dot(token_rows.T, up_back, preferred_element_type=jnp.float32).astype(jnp.bfloat16)
    down_grad = jnp.dot(hidden.T, out_scaled, preferred_element_type=jnp.float32).astype(jnp.bfloat16)
    slots = token_rows.shape[0]
    group = FF // N_TP
    gate_blocks = gate_back.astype(jnp.float32).reshape(slots, N_TP, group)
    up_blocks = up_back.astype(jnp.float32).reshape(slots, N_TP, group)
    terms = jnp.einsum('rtf,dtf->trd', gate_blocks, w_gate.astype(jnp.float32).reshape(D, N_TP, group))
    terms = terms + jnp.einsum('rtf,dtf->trd', up_blocks, w_up.astype(jnp.float32).reshape(D, N_TP, group))
    rounded = lax.optimization_barrier(terms.astype(jnp.bfloat16)).astype(jnp.float32)
    token_slots = lax.optimization_barrier(jnp.sum(rounded, axis=0)).astype(jnp.bfloat16)
    return (gate_grad, up_grad, down_grad, token_slots, mix_part)

def to_experts(rows):
    shaped = rows.reshape((N_EP, EXPERTS, CAP) + rows.shape[2:])
    return jnp.swapaxes(shaped, 0, 1).reshape((EXPERTS, N_EP * CAP) + rows.shape[2:])

def to_home(rows):
    shaped = rows.reshape((EXPERTS, N_EP, CAP) + rows.shape[2:])
    return jnp.swapaxes(shaped, 0, 1).reshape((N_EP, EXPERTS * CAP) + rows.shape[2:])

def reference(tokens, routes, router_matrix, cotangent, gate_proj, up_proj, down_proj):
    entries = TOK_DEV * TOP
    home_routes = routes.reshape(N_EP, entries)
    places, filler = jax.vmap(lambda flat: slot_places(flat, EXPERTS, CAP))(home_routes)
    occupied = filler < entries
    offsets = (jnp.arange(N_EP, dtype=jnp.int32) * TOK_DEV)[:, None]
    source = (jnp.where(occupied, filler // TOP, 0) + offsets).astype(jnp.int32)
    entry_src = (jnp.where(occupied, filler, 0) + offsets * TOP).astype(jnp.int32)
    logits = jnp.dot(tokens, router_matrix, preferred_element_type=jnp.float32)
    picked = routes[:, :, None] == jnp.arange(EXPERTS, dtype=jnp.int32)[None, None, :]
    chosen = lax.optimization_barrier(jnp.sum(jnp.where(picked, logits[:, None, :], jnp.float32(0.0)), axis=2))
    mixing = jax.nn.sigmoid(chosen - chosen[:, ::-1])
    token_slots = jnp.where(occupied[:, :, None], tokens[source], jnp.zeros((), jnp.bfloat16))
    output_slots = jnp.where(occupied[:, :, None], cotangent[source], jnp.zeros((), jnp.bfloat16))
    mix_slots = jnp.where(occupied, mixing.reshape(-1)[entry_src], jnp.float32(0.0)).astype(jnp.bfloat16)
    results = lax.map(expert_pass, (to_experts(token_slots), to_experts(output_slots), to_experts(mix_slots), gate_proj, up_proj, down_proj))
    gate_grad, up_grad, down_grad, back_slots, back_mix = results
    pick_rows = jax.vmap(lambda rows, where_at: rows[where_at])
    token_part = lax.optimization_barrier(jnp.sum(pick_rows(to_home(back_slots), places).reshape(TOKENS, TOP, D).astype(jnp.float32), axis=1))
    mixing_grad = pick_rows(to_home(back_mix), places).reshape(TOKENS, TOP)
    pairwise = mixing[:, 0] * mixing[:, 1]
    logit_grad = pairwise[:, None] * (mixing_grad - mixing_grad[:, ::-1])
    route_grad = lax.optimization_barrier(jnp.sum(jnp.where(picked, logit_grad[:, :, None], jnp.float32(0.0)), axis=1))
    router_path = jnp.dot(route_grad, router_matrix.astype(jnp.float32).T, precision=lax.Precision.HIGHEST)
    token_grad = (token_part + router_path).astype(jnp.bfloat16)
    router_grad = jnp.dot(tokens.astype(jnp.float32).T, route_grad, precision=lax.Precision.HIGHEST) * (1.0 / math.sqrt(TOKENS))
    return (token_grad, mixing_grad, router_grad, gate_grad, up_grad, down_grad)
```

```python
import math

import jax
import jax.numpy as jnp
from jax import lax
from jax.experimental import pallas as pl
from jax.experimental.pallas import tpu as pltpu
from jax.sharding import PartitionSpec as P

MESH = pl.DeviceIdType.MESH
BF16 = jnp.bfloat16
F32 = jnp.float32

NX, NY = 4, 4
OVER_ROWS = (((0,), (0,)), ((), ()))
OVER_COLS = (((1,), (1,)), ((), ()))


def dot(a, b, dims=None):
    if dims is None:
        return jnp.dot(a, b, preferred_element_type=F32)
    return lax.dot_general(a, b, dims, preferred_element_type=F32)


def iota(shape, dim):
    return lax.broadcasted_iota(jnp.int32, shape, dim)


def halves(value):
    high = value.astype(BF16)
    return high, (value - high.astype(F32)).astype(BF16)


def kernel(
    n_ep, n_tp,
    tokens_h, routes_ref, router_h, cot_h, gate_h, up_h, down_h,
    token_grad_ref, mixing_ref, router_grad_ref, gate_grad_ref, up_grad_ref, down_grad_ref,
    tok, cot, router, wtmp_g, wtmp_u, w2, wd,
    send, ms_send_buf, two_hot, small, gathered, ms_in,
    pre_g, pre_u, back, hid, hid_t, gu, ms_col, mix_col,
    terms, pair_in, near_a, near_b, far_p, far_m, total, ret_in,
    mix_row, mix_all, mix_tot, mix_in, mix_mat, rparts, rin,
    lsem,
    ms_s, ms_r, a2a_s, a2a_r, up_s, up_r, dn_s, dn_r, two_up_s, two_dn_s, two_r, pr_s, pr_r,
    ra_s, ra_r, rb_s, rb_r, rc_s, rc_r, rd_s, rd_r, re_s, re_r,
    mt_s, mt_r, mx_s, mx_r, rt_s, rt_r, ret_s, ret_r,
):
    nz = n_ep // NX
    rows, width = tok.shape
    experts = router.shape[1]
    cap = rows * 2 * 2 // experts
    cols = width // n_tp
    hidden = wtmp_g.shape[1]
    hpad = wd.shape[0]
    slots = experts * cap
    group = NX * cap
    chunk = 2 * group
    chunks = nz // 2
    ep, tp = lax.axis_index("ep"), lax.axis_index("tp")
    z, x = ep // NX, lax.rem(ep, NX)
    y, core = tp // 2, lax.rem(tp, 2)
    offsets = [0]
    for d in range(1, nz // 2 + 1):
        offsets += [d, -d] if d < nz // 2 else [d]

    def ring(value, step, size):
        return lax.rem(value + (step + size), size)

    def tp_of(step):
        return ring(y, step, NY) * 2 + core

    tp_up, tp_dn, tp_far = tp_of(1), tp_of(-1), tp_of(2)
    partner = y * 2 + (1 - core)

    def rcopy(src, dst, s, r, e, t):
        return pltpu.make_async_remote_copy(
            src_ref=src, dst_ref=dst, send_sem=s, recv_sem=r, device_id=(e, t), device_id_type=MESH
        )

    def wait_in(ref, s, r):
        rcopy(ref, ref, s, r, ep, partner).wait_recv()

    def wait_out(ref, s, r):
        rcopy(ref, ref, s, r, ep, partner).wait_send()

    ep_peers = []
    for g, dz in enumerate(offsets):
        for dx in range(NX):
            if dz or dx:
                ep_peers.append((g, ring(z, -dz, nz), ring(x, dx, NX)))

    barrier = pltpu.get_barrier_semaphore()
    for _, pz, px in ep_peers:
        pl.semaphore_signal(barrier, inc=1, device_id=(pz * NX + px, tp), device_id_type=MESH)
    for d in range(1, n_tp):
        pl.semaphore_signal(barrier, inc=1, device_id=(ep, ring(tp, d, n_tp)), device_id_type=MESH)
    loads = [
        pltpu.make_async_copy(a, b, lsem.at[k])
        for k, (a, b) in enumerate(
            (
                (tokens_h, tok), (router_h, router), (cot_h, cot), (gate_h.at[0], wtmp_g),
                (up_h.at[0], wtmp_u), (down_h.at[0], wd.at[pl.ds(0, hidden)]),
            )
        )
    ]
    for load in loads:
        load.start()
    w2[...] = jnp.zeros_like(w2)
    wd[pl.ds(hidden, hpad - hidden), :] = jnp.zeros((hpad - hidden, width), BF16)
    loads[0].wait()
    loads[1].wait()

    lanes = iota((rows, 128), 1)
    r0, r1 = routes_ref[:, 0:1], routes_ref[:, 1:2]
    oh0, oh1 = r0 == lanes, r1 == lanes
    both = jnp.where(oh0 | oh1, 1.0, 0.0).astype(BF16)
    before = jnp.where(iota((rows, rows), 0) > iota((rows, rows), 1), 1.0, 0.0).astype(BF16)
    earlier = dot(before, both)
    rank0 = jnp.sum(jnp.where(oh0, earlier, 0.0), axis=1, keepdims=True)
    rank1 = jnp.sum(jnp.where(oh1, earlier, 0.0), axis=1, keepdims=True)
    logits = dot(tok[...], router[...])
    lane_e = iota((rows, experts), 1)
    chosen0 = jnp.sum(jnp.where(r0 == lane_e, logits, 0.0), axis=1, keepdims=True)
    chosen1 = jnp.sum(jnp.where(r1 == lane_e, logits, 0.0), axis=1, keepdims=True)
    mix0 = jax.nn.sigmoid(chosen0 - chosen1)
    mix1 = jax.nn.sigmoid(chosen1 - chosen0)
    small[:, 0:1] = rank0
    small[:, 1:2] = rank1
    small[:, 2:3] = mix0
    small[:, 3:4] = mix1
    place0 = r0.astype(F32) * cap + rank0
    place1 = r1.astype(F32) * cap + rank1
    mb0 = mix0.astype(BF16).astype(F32)
    mb1 = mix1.astype(BF16).astype(F32)
    loads[2].wait()
    source = jnp.concatenate(
        [tok[:, pl.ds(pl.multiple_of(tp * cols, cols), cols)], cot[...]], axis=1
    )
    for k in range(slots // 128):
        at = (iota((rows, 128), 1) + k * 128).astype(F32)
        hit0, hit1 = place0 == at, place1 == at
        chosen = jnp.where(hit0 | hit1, 1.0, 0.0).astype(BF16)
        two_hot[:, k * 128 : (k + 1) * 128] = chosen
        ms_send_buf[k] = jnp.sum(
            jnp.where(hit0, mb0, 0.0) + jnp.where(hit1, mb1, 0.0), axis=0, keepdims=True
        )
        picked = dot(chosen, source, OVER_ROWS).astype(BF16)
        for m in range(128 // cap):
            send[k * (128 // cap) + m] = picked[m * cap : (m + 1) * cap]

    pl.semaphore_wait(barrier, len(ep_peers) + n_tp - 1)

    own_rows = pl.ds(pl.multiple_of(x * cap, cap), cap)
    for g, pz, px in ep_peers:
        rcopy(ms_send_buf.at[pz], ms_in.at[g * NX + x], ms_s, ms_r, pz * NX + px, tp).start()
        rcopy(
            send.at[pz * NX + px], gathered.at[tp, g, own_rows], a2a_s, a2a_r.at[g], pz * NX + px, tp
        ).start()
    gathered[tp, 0, own_rows, :] = send[ep]
    ms_in[x] = ms_send_buf[z]
    for k, wtmp in ((3, wtmp_g), (4, wtmp_u)):
        loads[k].wait()

        def place(i, carry, wtmp=wtmp, at=(k - 3) * hpad):
            block = pl.ds(pl.multiple_of(i * 128, 128), 128)
            w2[block, at : at + hidden] = wtmp[block, :]
            return carry

        lax.fori_loop(0, width // 128, place, 0)
    loads[5].wait()

    def to_partner(share, g):
        piece = gathered.at[share, g]
        rcopy(piece, piece, pr_s, pr_r.at[g], ep, partner).start()

    def stage1(g):
        if g == 0:
            wait_in(gathered.at[tp, 0, pl.ds(0, group - cap)], a2a_s, a2a_r.at[0])
        else:
            wait_in(gathered.at[tp, g], a2a_s, a2a_r.at[g])
        piece = gathered.at[tp, g]
        rcopy(piece, piece, up_s, up_r.at[g], ep, tp_up).start()
        rcopy(piece, piece, dn_s, dn_r.at[g], ep, tp_dn).start()
        to_partner(tp, g)

    def stage2(g):
        below, above = gathered.at[tp_dn, g], gathered.at[tp_up, g]
        wait_in(below, up_s, up_r.at[g])
        if g % 2 == 0:
            rcopy(below, below, two_up_s, two_r.at[g], ep, tp_up).start()
        to_partner(tp_dn, g)
        wait_in(above, dn_s, dn_r.at[g])
        if g % 2 == 1:
            rcopy(above, above, two_dn_s, two_r.at[g], ep, tp_dn).start()
        to_partner(tp_up, g)

    def stage3(g):
        wait_in(gathered.at[tp_far, g], two_up_s, two_r.at[g])
        to_partner(tp_far, g)

    def stage4(g):
        wait_in(gathered.at[pl.ds(0, NY), g], pr_s, pr_r.at[g])

    def compute(q):
        at = slice(2 * q, 2 * q + 2)

        def part(k, lo):
            return gathered[k, at, :, lo : lo + cols].reshape(chunk, cols)

        xs = jnp.concatenate([part(k, 0) for k in range(n_tp)], axis=1)
        pre_g[...] = dot(xs, w2[:, :hpad])
        pre_u[...] = dot(xs, w2[:, hpad:])
        ys = jnp.concatenate([part(k, cols) for k in range(n_tp)], axis=1)
        back[...] = dot(ys, wd[...], OVER_COLS)
        if q == 0:
            wait_in(ms_in.at[pl.ds(0, n_ep - 1)], ms_s, ms_r)
        mine = iota((cap, 128), 1) == iota((cap, 128), 0) + x * cap
        spread = jnp.where(mine[None], ms_in[2 * q * NX : (2 * q + 2) * NX], 0.0)
        ms_col[pl.ds(q * chunk, chunk), :] = jnp.sum(spread, axis=2, keepdims=True).reshape(chunk, 1)

        def element(i, carry):
            block = pl.ds(pl.multiple_of(i * 32, 32), 32)
            out = pl.ds(pl.multiple_of(q * chunk + i * 32, 32), 32)
            a, u, b = pre_g[block, :], pre_u[block, :], back[block, :]
            sig = jax.nn.sigmoid(a)
            active = a * sig
            h = (active * u).astype(BF16)
            hid[block, :] = h
            mix_col[block, :] = jnp.sum(h.astype(F32) * b, axis=1, keepdims=True)
            scaled = ms_col[out, :] * b
            gu[out, :hpad] = (scaled * u * sig * (1.0 + a * (1.0 - sig))).astype(BF16)
            gu[out, hpad:] = (scaled * active).astype(BF16)
            return carry

        lax.fori_loop(0, chunk // 32, element, 0)
        eye = iota((group, group), 0) == iota((group, group), 1)
        for m in range(2):
            column = mix_col[m * group : (m + 1) * group, :]
            mix_row[2 * q + m] = jnp.sum(jnp.where(eye, column, 0.0), axis=0, keepdims=True)
        hid_t[:, q * chunk : (q + 1) * chunk] = hid[...].T

        def term(k, carry):
            w = w2[pl.ds(pl.multiple_of(k * cols, cols), cols), :]
            t = dot(gu[pl.ds(q * chunk, chunk), :], w, OVER_COLS)
            terms[lax.rem(k, 2), k // 2, at] = t.astype(BF16).reshape(2, group, cols)
            return carry

        lax.fori_loop(0, n_tp, term, 0)

    def rs_a(q):
        both_g = pl.ds(2 * q, 2)
        rcopy(terms.at[1 - core, :, both_g], pair_in.at[:, both_g], ra_s, ra_r.at[q], ep, partner).start()

    def add_into(ref, index, other):
        ref[index] = (ref[index].astype(F32) + other.astype(F32)).astype(BF16)

    yu, yd, yf = ring(y, 1, NY), ring(y, -1, NY), ring(y, 2, NY)

    def rs_bc(q):
        both_g = pl.ds(2 * q, 2)
        wait_in(pair_in.at[:, both_g], ra_s, ra_r.at[q])
        for k in (yf, yu, yd, y):
            for g in (2 * q, 2 * q + 1):
                add_into(terms, (core, k, g), pair_in[k, g])
        rcopy(terms.at[core, yf, 2 * q], near_a.at[q], rb_s, rb_r.at[q], ep, tp_up).start()
        rcopy(terms.at[core, yf, 2 * q + 1], near_b.at[q], rc_s, rc_r.at[q], ep, tp_dn).start()

    def rs_de(q):
        both_g = pl.ds(2 * q, 2)
        wait_in(near_a.at[q], rb_s, rb_r.at[q])
        add_into(terms, (core, yu, 2 * q), near_a[q])
        rcopy(terms.at[core, yu, both_g], far_p.at[both_g], rd_s, rd_r.at[q], ep, tp_up).start()
        wait_in(near_b.at[q], rc_s, rc_r.at[q])
        add_into(terms, (core, yd, 2 * q + 1), near_b[q])
        rcopy(terms.at[core, yd, both_g], far_m.at[both_g], re_s, re_r.at[q], ep, tp_dn).start()

    def rs_fg(q):
        both_g = pl.ds(2 * q, 2)
        wait_in(far_p.at[both_g], rd_s, rd_r.at[q])
        wait_in(far_m.at[both_g], re_s, re_r.at[q])
        for g in (2 * q, 2 * q + 1):
            summed = terms[core, y, g].astype(F32) + far_p[g].astype(F32) + far_m[g].astype(F32)
            total[g] = summed.astype(BF16)
            for dx in range(NX):
                if not (g or dx):
                    continue
                pz, px = ring(z, offsets[g], nz), ring(x, dx, NX)
                piece = total.at[g, pl.ds(pl.multiple_of(px * cap, cap), cap)]
                rcopy(piece, ret_in.at[ep], ret_s, ret_r, pz * NX + px, tp).start()
        if q == 0:
            ret_in[ep] = total[0, own_rows, :]

    def weights(k, carry):
        def all_rows(lo):
            return gathered[k, :, :, lo : lo + cols].reshape(slots, cols)

        at = pl.ds(pl.multiple_of(k * cols, cols), cols)
        both_grads = dot(all_rows(0), gu[...], OVER_ROWS)
        gate_grad_ref[at, :] = both_grads[:, :hidden].astype(BF16)
        up_grad_ref[at, :] = both_grads[:, hpad : hpad + hidden].astype(BF16)
        scaled = (ms_col[...] * all_rows(cols).astype(F32)).astype(BF16)
        down_grad_ref[:, at] = dot(hid_t[...], scaled)[:hidden].astype(BF16)
        return carry

    for s in range(nz + 3):
        if s < nz:
            stage1(s)
        if 0 <= s - 1 < nz:
            stage2(s - 1)
        if 0 <= s - 2 < nz:
            stage3(s - 2)
        if 0 <= s - 3 < nz:
            stage4(s - 3)
            if (s - 3) % 2:
                q = (s - 3) // 2
                compute(q)
                rs_a(q)
                if q >= 1:
                    rs_bc(q - 1)
                if q >= 2:
                    rs_de(q - 2)
                if q >= 3:
                    rs_fg(q - 3)

    mix_all[tp] = mix_row[...]
    for d in range(1, n_tp):
        rcopy(mix_row, mix_all.at[tp], mt_s, mt_r, ep, ring(tp, d, n_tp)).start()
    piece_k = n_tp // 4
    rs_bc(chunks - 1)
    rs_de(chunks - 2)
    lax.fori_loop(0, piece_k, weights, 0)
    rs_fg(chunks - 3)
    wait_in(mix_all.at[pl.ds(0, n_tp - 1)], mt_s, mt_r)
    mix_sum = mix_all[0]
    for k in range(1, n_tp):
        mix_sum = mix_sum + mix_all[k]
    mix_tot[...] = mix_sum
    mix_in[ep] = mix_tot[0]
    for g, dz in enumerate(offsets):
        for dx in range(NX):
            if g or dx:
                peer = ring(z, dz, nz) * NX + ring(x, dx, NX)
                rcopy(mix_tot.at[g], mix_in.at[ep], mx_s, mx_r, peer, tp).start()
    rs_de(chunks - 1)
    rs_fg(chunks - 2)
    lax.fori_loop(piece_k, 2 * piece_k, weights, 0)
    rs_fg(chunks - 1)

    wait_in(mix_in.at[pl.ds(0, n_ep - 1)], mx_s, mx_r)
    for e in range(n_ep):
        mix_mat[e : e + 1, :] = mix_in[e]
    rank0, rank1, mix0, mix1 = (small[:, k : k + 1] for k in range(4))
    r0, r1 = routes_ref[:, 0:1], routes_ref[:, 1:2]
    lane_f = (lanes - x * cap).astype(F32)
    lane_e = iota((rows, experts), 1)

    def own_grad(route, rank):
        chosen = jnp.where(route == lane_e, 1.0, 0.0)
        spread = lax.dot_general(
            chosen, mix_mat[...], (((1,), (0,)), ((), ())),
            precision=lax.Precision.HIGHEST, preferred_element_type=F32,
        )
        return jnp.sum(jnp.where(rank == lane_f, spread, 0.0), axis=1, keepdims=True)

    grad0, grad1 = own_grad(r0, rank0), own_grad(r1, rank1)
    mixing_ref[:, 0:1] = grad0
    mixing_ref[:, 1:2] = grad1
    pairwise = mix0 * mix1
    route_grad = jnp.where(r0 == lanes, pairwise * (grad0 - grad1), 0.0)
    route_grad = route_grad + jnp.where(r1 == lanes, pairwise * (grad1 - grad0), 0.0)
    rg_hi, rg_lo = halves(route_grad)
    scale = 1.0 / math.sqrt(rows * n_ep)

    def router_part(k, carry):
        at = pl.ds(pl.multiple_of(k * cols, cols), cols)
        t = tok[:, at]
        rparts[at, :] = (dot(t, rg_hi, OVER_ROWS) + dot(t, rg_lo, OVER_ROWS)) * scale
        return carry

    lax.fori_loop(0, n_tp, router_part, 0)
    share = width // (n_ep * n_tp)

    def share_rows(e):
        return pl.ds(pl.multiple_of((e * n_tp + tp) * share, share), share)

    for _, pz, px in ep_peers:
        peer = pz * NX + px
        rcopy(rparts.at[share_rows(peer)], rin.at[ep], rt_s, rt_r, peer, tp).start()
    rin[ep] = rparts[share_rows(ep), :]
    router_rows = router[pl.ds(pl.multiple_of(tp * cols, cols), cols), :]
    path = dot(rg_hi[:, :experts], router_rows, OVER_COLS)
    path = path + dot(rg_lo[:, :experts], router_rows, OVER_COLS)
    lax.fori_loop(2 * piece_k, n_tp, weights, 0)

    wait_in(ret_in.at[pl.ds(0, n_ep - 1)], ret_s, ret_r)
    token_part = dot(two_hot[...], ret_in[...].reshape(slots, cols))
    token_grad_ref[...] = (token_part + path).astype(BF16)
    wait_in(rin.at[pl.ds(0, n_ep - 1)], rt_s, rt_r)
    acc = rin[0]
    for e in range(1, n_ep):
        acc = acc + rin[e]
    router_grad_ref[...] = acc[:, :experts]

    wait_out(ms_in.at[pl.ds(0, n_ep - 1)], ms_s, ms_r)
    wait_out(send.at[pl.ds(0, n_ep - 1)], a2a_s, a2a_r.at[0])
    wait_out(gathered.at[0], up_s, up_r.at[0])
    wait_out(gathered.at[0], dn_s, dn_r.at[0])
    wait_out(gathered.at[0, pl.ds(0, nz // 2)], two_up_s, two_r.at[0])
    wait_out(gathered.at[0, pl.ds(0, nz // 2)], two_dn_s, two_r.at[0])
    wait_out(gathered.at[pl.ds(0, NY)], pr_s, pr_r.at[0])
    wait_out(pair_in, ra_s, ra_r.at[0])
    wait_out(near_a, rb_s, rb_r.at[0])
    wait_out(near_b, rc_s, rc_r.at[0])
    wait_out(far_p, rd_s, rd_r.at[0])
    wait_out(far_m, re_s, re_r.at[0])
    wait_out(mix_all.at[pl.ds(0, n_tp - 1)], mt_s, mt_r)
    wait_out(mix_in.at[pl.ds(0, n_ep - 1)], mx_s, mx_r)
    wait_out(rin.at[pl.ds(0, n_ep - 1)], rt_s, rt_r)
    wait_out(ret_in.at[pl.ds(0, n_ep - 1)], ret_s, ret_r)


def solution(mesh):
    n_ep, n_tp = mesh.shape["ep"], mesh.shape["tp"]

    def local(tokens, routes, router_matrix, cotangent, gate_proj, up_proj, down_proj):
        rows, width = tokens.shape
        experts = router_matrix.shape[1]
        hidden = gate_proj.shape[2]
        hpad = -(-hidden // 128) * 128
        cap = rows * 2 * 2 // experts
        slots = experts * cap
        cols = width // n_tp
        nz = n_ep // NX
        group = NX * cap
        chunk, chunks = 2 * group, nz // 2
        share = width // (n_ep * n_tp)
        dma = pltpu.SemaphoreType.DMA
        vmem = pltpu.VMEM
        any_ = pl.BlockSpec(memory_space=pl.ANY)
        whole = pl.BlockSpec(memory_space=pltpu.VMEM)
        scratch = [
            vmem((rows, width), BF16), vmem((rows, cols), BF16), vmem((width, experts), BF16),
            vmem((width, hidden), BF16), vmem((width, hidden), BF16),
            vmem((width, 2 * hpad), BF16), vmem((hpad, width), BF16),
            vmem((n_ep, cap, 2 * cols), BF16), vmem((slots // 128, 1, 128), F32),
            vmem((rows, slots), BF16), vmem((rows, 128), F32),
            vmem((n_tp, nz, group, 2 * cols), BF16), vmem((n_ep, 1, 128), F32),
            vmem((chunk, hpad), F32), vmem((chunk, hpad), F32), vmem((chunk, hpad), F32),
            vmem((chunk, hpad), BF16), vmem((hpad, slots), BF16), vmem((slots, 2 * hpad), BF16),
            vmem((slots, 1), F32), vmem((chunk, 1), F32),
            vmem((2, NY, nz, group, cols), BF16), vmem((NY, nz, group, cols), BF16),
            vmem((chunks, group, cols), BF16), vmem((chunks, group, cols), BF16),
            vmem((nz, group, cols), BF16), vmem((nz, group, cols), BF16),
            vmem((nz, group, cols), BF16), vmem((n_ep, cap, cols), BF16),
            vmem((nz, 1, 128), F32), vmem((n_tp, nz, 1, 128), F32), vmem((nz, 1, 128), F32),
            vmem((n_ep, 1, 128), F32), vmem((n_ep, 128), F32),
            vmem((width, 128), F32), vmem((n_ep, share, 128), F32),
            dma((6,)),
            dma, dma, dma, dma((nz,)), dma, dma((nz,)), dma, dma((nz,)), dma, dma, dma((nz,)),
            dma, dma((nz,)),
            dma, dma((chunks,)), dma, dma((chunks,)), dma, dma((chunks,)), dma, dma((chunks,)),
            dma, dma((chunks,)),
            dma, dma, dma, dma, dma, dma, dma, dma,
        ]
        shape = jax.ShapeDtypeStruct
        token_grad, mixing, router_grad, gate_grad, up_grad, down_grad = pl.pallas_call(
            lambda *refs: kernel(n_ep, n_tp, *refs),
            out_shape=(
                shape((rows, cols), BF16), shape((rows, 2), F32), shape((share, experts), F32),
                shape((width, hidden), BF16), shape((width, hidden), BF16),
                shape((hidden, width), BF16),
            ),
            in_specs=[any_, whole, any_, any_, any_, any_, any_],
            out_specs=(whole,) * 6,
            scratch_shapes=scratch,
            compiler_params=pltpu.CompilerParams(
                collective_id=0, has_side_effects=True, vmem_limit_bytes=66 * 1024 * 1024 - 2**21
            ),
            name="moe_backward",
        )(tokens, routes, router_matrix, cotangent, gate_proj, up_proj, down_proj)
        return token_grad, mixing, router_grad, gate_grad[None], up_grad[None], down_grad[None]

    return jax.shard_map(
        local,
        mesh=mesh,
        in_specs=(
            P("ep", None), P("ep", None), P(), P("ep", "tp"),
            P("ep", None, "tp"), P("ep", None, "tp"), P("ep", "tp", None),
        ),
        out_specs=(
            P("ep", "tp"), P("ep", None), P(("ep", "tp"), None),
            P("ep", None, "tp"), P("ep", None, "tp"), P("ep", "tp", None),
        ),
        check_vma=False,
    )
```

```python
import math

import jax
import jax.numpy as jnp
from jax import lax
from jax.experimental import pallas as pl
from jax.experimental.pallas import tpu as pltpu
from jax.sharding import PartitionSpec as P

MESH = pl.DeviceIdType.MESH
BF16 = jnp.bfloat16
F32 = jnp.float32

NX, NY = 4, 4
OFFSETS = (0, 1, -2, 3, -3, 4, -1, 2)
VMEM_LIMIT = 47 * 2**20
OVER_ROWS = (((0,), (0,)), ((), ()))
OVER_COLS = (((1,), (1,)), ((), ()))


def dot(a, b, dims=None):
    if dims is None:
        return jnp.dot(a, b, preferred_element_type=F32)
    return lax.dot_general(a, b, dims, preferred_element_type=F32)


def iota(shape, dim):
    return lax.broadcasted_iota(jnp.int32, shape, dim)


def phase(step):
    def named(k):
        with jax.named_scope(step.__name__ + str(k)):
            return step(k)

    return named


def halves(value):
    high = value.astype(BF16)
    return high, (value - high.astype(F32)).astype(BF16)


def kernel(
    n_ep, n_tp, hidden,
    tokens_h, routes_ref, router_h, cot_h, gate_h, up_h, down_h,
    token_grad_ref, mixing_ref, router_grad_ref, gate_grad_ref, up_grad_ref, down_grad_ref,
    tok, cot, router, w2, wd, w2_t, wd_t,
    send, ms_send_buf, two_hot, small, gathered, ms_in,
    pre, back, hid, hid_t, gu, gu_t, ms_col, mix_col,
    terms, pair_in, near_a, near_b, far_p, far_m, total, ret_in,
    mix_row, mix_all, mix_tot, mix_in, mix_mat, rparts, rin,
    lsem,
    ms_s, ms_r, a2a_s, a2a_r, up_s, up_r, dn_s, dn_r, two_up_s, two_dn_s, two_r, pr_s, pr_r,
    ra_s, ra_r, rb_s, rb_r, rc_s, rc_r, rd_s, rd_r, re_s, re_r,
    mt_s, mt_r, mx_s, mx_r, rt_s, rt_r, ret_s, ret_r,
):
    nz = n_ep // NX
    rows, width = tok.shape
    experts = router.shape[0]
    cap = rows * 2 * 2 // experts
    cols = width // n_tp
    hpad = wd.shape[0]
    slots = experts * cap
    group = NX * cap
    chunk = 2 * group
    chunks = nz // 2
    ep, tp = lax.axis_index("ep"), lax.axis_index("tp")
    z, x = ep // NX, lax.rem(ep, NX)
    y, core = tp // 2, lax.rem(tp, 2)
    offsets = OFFSETS
    home = offsets.index(0)

    def ring(value, step, size):
        return lax.rem(value + (step + size), size)

    def tp_of(step):
        return ring(y, step, NY) * 2 + core

    tp_up, tp_dn, tp_far = tp_of(1), tp_of(-1), tp_of(2)
    partner = y * 2 + (1 - core)

    def rcopy(src, dst, s, r, e, t):
        return pltpu.make_async_remote_copy(
            src_ref=src, dst_ref=dst, send_sem=s, recv_sem=r, device_id=(e, t), device_id_type=MESH
        )

    def wait_in(ref, s, r):
        rcopy(ref, ref, s, r, ep, partner).wait_recv()

    def wait_out(ref, s, r):
        rcopy(ref, ref, s, r, ep, partner).wait_send()

    ep_peers = []
    for g, dz in enumerate(offsets):
        for dx in range(NX):
            if dz or dx:
                ep_peers.append((g, ring(z, -dz, nz), ring(x, dx, NX)))

    barrier = pltpu.get_barrier_semaphore()
    for _, pz, px in ep_peers:
        pl.semaphore_signal(barrier, inc=1, device_id=(pz * NX + px, tp), device_id_type=MESH)
    for d in range(1, n_tp):
        pl.semaphore_signal(barrier, inc=1, device_id=(ep, ring(tp, d, n_tp)), device_id_type=MESH)
    loads = [
        pltpu.make_async_copy(a, b, lsem.at[k])
        for k, (a, b) in enumerate(
            (
                (tokens_h, tok), (router_h, router), (cot_h, cot),
                (gate_h.at[0], w2.at[pl.ds(0, hidden)]),
                (up_h.at[0], w2.at[pl.ds(hpad, hidden)]),
                (down_h.at[0], wd.at[pl.ds(0, hidden)]),
            )
        )
    ]
    for load in loads:
        load.start()
    gap = jnp.zeros((hpad - hidden, width), BF16)
    w2[hidden:hpad, :] = gap
    w2[hpad + hidden :, :] = gap
    wd[hidden:, :] = gap
    with jax.named_scope("load"):
        loads[0].wait()
        loads[1].wait()

    lanes = iota((rows, 128), 1)
    diagonal = iota((rows, rows), 0) == iota((rows, rows), 1)

    def column(row):
        return jnp.sum(jnp.where(diagonal, row, 0.0), axis=1, keepdims=True)

    r0, r1 = (column(routes_ref[k : k + 1, :].astype(F32)) for k in range(2))
    lanes_f = lanes.astype(F32)
    oh0, oh1 = r0 == lanes_f, r1 == lanes_f
    both = jnp.where(oh0 | oh1, 1.0, 0.0).astype(BF16)
    before = jnp.where(iota((rows, rows), 0) > iota((rows, rows), 1), 1.0, 0.0).astype(BF16)
    earlier = dot(before, both)
    rank0 = jnp.sum(jnp.where(oh0, earlier, 0.0), axis=1, keepdims=True)
    rank1 = jnp.sum(jnp.where(oh1, earlier, 0.0), axis=1, keepdims=True)
    logits = dot(tok[...], router[...], OVER_COLS)
    lane_e = iota((rows, experts), 1).astype(F32)
    chosen0 = jnp.sum(jnp.where(r0 == lane_e, logits, 0.0), axis=1, keepdims=True)
    chosen1 = jnp.sum(jnp.where(r1 == lane_e, logits, 0.0), axis=1, keepdims=True)
    mix0 = jax.nn.sigmoid(chosen0 - chosen1)
    mix1 = jax.nn.sigmoid(chosen1 - chosen0)
    small[:, 0:1] = rank0
    small[:, 1:2] = rank1
    small[:, 2:3] = mix0
    small[:, 3:4] = mix1
    small[:, 4:5] = r0
    small[:, 5:6] = r1
    place0 = r0 * cap + rank0
    place1 = r1 * cap + rank1
    mb0 = mix0.astype(BF16).astype(F32)
    mb1 = mix1.astype(BF16).astype(F32)
    loads[2].wait()
    source = jnp.concatenate(
        [tok[:, pl.ds(pl.multiple_of(tp * cols, cols), cols)], cot[...]], axis=1
    )
    for k in range(slots // 128):
        at = (iota((rows, 128), 1) + k * 128).astype(F32)
        hit0, hit1 = place0 == at, place1 == at
        chosen = jnp.where(hit0 | hit1, 1.0, 0.0).astype(BF16)
        two_hot[:, k * 128 : (k + 1) * 128] = chosen
        ms_send_buf[k] = jnp.sum(
            jnp.where(hit0, mb0, 0.0) + jnp.where(hit1, mb1, 0.0), axis=0, keepdims=True
        )
        picked = dot(chosen, source, OVER_ROWS).astype(BF16)
        for m in range(128 // cap):
            send[k * (128 // cap) + m] = picked[m * cap : (m + 1) * cap]

    with jax.named_scope("barrier"):
        pl.semaphore_wait(barrier, len(ep_peers) + n_tp - 1)

    own_rows = pl.ds(pl.multiple_of(x * cap, cap), cap)
    for g, pz, px in ep_peers:
        peer, land = pz * NX + px, gathered.at[tp, g, own_rows]
        rcopy(ms_send_buf.at[pz], ms_in.at[g * NX + x], ms_s, ms_r, peer, tp).start()
        rcopy(send.at[peer], land, a2a_s, a2a_r.at[g], peer, tp).start()
    gathered[tp, home, own_rows, :] = send[ep]
    ms_in[home * NX + x] = ms_send_buf[z]
    with jax.named_scope("weights_in"):
        for load in loads[3:]:
            load.wait()

        def flip(k, carry):
            at = pl.ds(pl.multiple_of(k * cols, cols), cols)
            w2_t[at, :] = w2[:, at].T
            wd_t[at, :] = wd[:, at].T
            return carry

        lax.fori_loop(0, n_tp, flip, 0)

    def to_partner(share, g):
        piece = gathered.at[share, g]
        rcopy(piece, piece, pr_s, pr_r.at[g], ep, partner).start()

    @phase
    def stage1(g):
        if g == home:
            wait_in(gathered.at[tp, g, pl.ds(0, group - cap)], a2a_s, a2a_r.at[g])
        else:
            wait_in(gathered.at[tp, g], a2a_s, a2a_r.at[g])
        piece = gathered.at[tp, g]
        rcopy(piece, piece, up_s, up_r.at[g], ep, tp_up).start()
        rcopy(piece, piece, dn_s, dn_r.at[g], ep, tp_dn).start()
        to_partner(tp, g)

    @phase
    def stage2(g):
        below, above = gathered.at[tp_dn, g], gathered.at[tp_up, g]
        wait_in(below, up_s, up_r.at[g])
        if g % 2 == 0:
            rcopy(below, below, two_up_s, two_r.at[g], ep, tp_up).start()
        to_partner(tp_dn, g)
        wait_in(above, dn_s, dn_r.at[g])
        if g % 2 == 1:
            rcopy(above, above, two_dn_s, two_r.at[g], ep, tp_dn).start()
        to_partner(tp_up, g)

    @phase
    def stage3(g):
        wait_in(gathered.at[tp_far, g], two_up_s, two_r.at[g])
        to_partner(tp_far, g)

    @phase
    def stage4(g):
        wait_in(gathered.at[pl.ds(0, NY), g], pr_s, pr_r.at[g])

    def rows_of(q, lo):
        at = slice(2 * q, 2 * q + 2)
        return jnp.concatenate(
            [gathered[k, at, :, lo : lo + cols].reshape(chunk, cols) for k in range(n_tp)], axis=1
        )

    @phase
    def forward(q):
        pre[...] = dot(rows_of(q, 0), w2_t[...])

    @phase
    def backward(q):
        back[...] = dot(rows_of(q, cols), wd_t[...])
        if q == 0:
            wait_in(ms_in.at[pl.ds(0, n_ep - 1)], ms_s, ms_r)
        mine = iota((cap, 128), 1) == iota((cap, 128), 0) + x * cap
        spread = jnp.where(mine[None], ms_in[2 * q * NX : (2 * q + 2) * NX], 0.0)
        ms_col[pl.ds(q * chunk, chunk), :] = jnp.sum(spread, axis=2, keepdims=True).reshape(chunk, 1)

    @phase
    def element(q):
        def block_of(i, carry):
            block = pl.ds(pl.multiple_of(i * 32, 32), 32)
            out = pl.ds(pl.multiple_of(q * chunk + i * 32, 32), 32)
            a, u, b = pre[block, :hpad], pre[block, hpad:], back[block, :]
            sig = jax.nn.sigmoid(a)
            active = a * sig
            h = (active * u).astype(BF16)
            hid[block, :] = h
            mix_col[block, :] = jnp.sum(h.astype(F32) * b, axis=1, keepdims=True)
            scaled = ms_col[out, :] * b
            gu[out, :hpad] = (scaled * u * sig * (1.0 + a * (1.0 - sig))).astype(BF16)
            gu[out, hpad:] = (scaled * active).astype(BF16)
            return carry

        lax.fori_loop(0, chunk // 32, block_of, 0)

    @phase
    def term(q):
        def term_of(k, carry):
            w = w2[:, pl.ds(pl.multiple_of(k * 4 * cols, 4 * cols), 4 * cols)]
            t = dot(gu[pl.ds(q * chunk, chunk), :], w).astype(BF16)
            for m in range(4):
                piece = t[:, m * cols : (m + 1) * cols].reshape(2, group, cols)
                terms[m % 2, 2 * k + m // 2, 2 * q : 2 * q + 2] = piece
            return carry

        lax.fori_loop(0, n_tp // 4, term_of, 0)

    @phase
    def turn(q):
        eye = iota((group, group), 0) == iota((group, group), 1)
        for m in range(2):
            column = mix_col[m * group : (m + 1) * group, :]
            mix_row[2 * q + m] = jnp.sum(jnp.where(eye, column, 0.0), axis=0, keepdims=True)
        hid_t[:, q * chunk : (q + 1) * chunk] = hid[...].T
        gu_t[:, q * chunk : (q + 1) * chunk] = gu[q * chunk : (q + 1) * chunk, :].T

    @phase
    def rs_a(q):
        both_g = pl.ds(2 * q, 2)
        rcopy(terms.at[1 - core, :, both_g], pair_in.at[:, both_g], ra_s, ra_r.at[q], ep, partner).start()

    def add_into(ref, index, other):
        ref[index] = (ref[index].astype(F32) + other.astype(F32)).astype(BF16)

    yu, yd, yf = ring(y, 1, NY), ring(y, -1, NY), ring(y, 2, NY)

    @phase
    def rs_bc(q):
        both_g = pl.ds(2 * q, 2)
        wait_in(pair_in.at[:, both_g], ra_s, ra_r.at[q])
        for k in (yf, yu, yd, y):
            for g in (2 * q, 2 * q + 1):
                add_into(terms, (core, k, g), pair_in[k, g])
        rcopy(terms.at[core, yf, 2 * q], near_a.at[q], rb_s, rb_r.at[q], ep, tp_up).start()
        rcopy(terms.at[core, yf, 2 * q + 1], near_b.at[q], rc_s, rc_r.at[q], ep, tp_dn).start()

    @phase
    def rs_de(q):
        both_g = pl.ds(2 * q, 2)
        wait_in(near_a.at[q], rb_s, rb_r.at[q])
        add_into(terms, (core, yu, 2 * q), near_a[q])
        rcopy(terms.at[core, yu, both_g], far_p.at[both_g], rd_s, rd_r.at[q], ep, tp_up).start()
        wait_in(near_b.at[q], rc_s, rc_r.at[q])
        add_into(terms, (core, yd, 2 * q + 1), near_b[q])
        rcopy(terms.at[core, yd, both_g], far_m.at[both_g], re_s, re_r.at[q], ep, tp_dn).start()

    @phase
    def rs_fg(q):
        both_g = pl.ds(2 * q, 2)
        wait_in(far_p.at[both_g], rd_s, rd_r.at[q])
        wait_in(far_m.at[both_g], re_s, re_r.at[q])
        for g in (2 * q, 2 * q + 1):
            summed = terms[core, y, g].astype(F32) + far_p[g].astype(F32) + far_m[g].astype(F32)
            total[g] = summed.astype(BF16)
            for dx in range(NX):
                if g == home and dx == 0:
                    continue
                pz, px = ring(z, offsets[g], nz), ring(x, dx, NX)
                piece = total.at[g, pl.ds(pl.multiple_of(px * cap, cap), cap)]
                rcopy(piece, ret_in.at[ep], ret_s, ret_r, pz * NX + px, tp).start()
        if q == home // 2:
            ret_in[ep] = total[home, own_rows, :]

    def weights(k, carry):
        def all_rows(lo):
            return gathered[k, :, :, lo : lo + cols].reshape(slots, cols)

        at = pl.ds(pl.multiple_of(k * cols, cols), cols)
        both_grads = dot(gu_t[...], all_rows(0)).astype(BF16)
        gate_grad_ref[:, at] = both_grads[:hidden]
        up_grad_ref[:, at] = both_grads[hpad : hpad + hidden]
        scaled = (ms_col[...] * all_rows(cols).astype(F32)).astype(BF16)
        down_grad_ref[:, at] = dot(hid_t[...], scaled)[:hidden].astype(BF16)
        return carry

    def poll(k):
        if k < nz:
            stage2(k)
        if k + 2 < nz:
            stage1(k + 2)
        if k:
            stage3(k - 1)

    def ready(q):
        stage4(2 * q)
        stage4(2 * q + 1)

    def grads(lo, hi):
        with jax.named_scope("grads" + str(lo)):
            lax.fori_loop(lo, hi, weights, 0)

    def mix_out(q):
        both_g = pl.ds(2 * q, 2)
        mix_all[tp, both_g] = mix_row[both_g]
        for d in range(1, n_tp):
            peer = ring(tp, d, n_tp)
            rcopy(mix_row.at[both_g], mix_all.at[tp, both_g], mt_s, mt_r.at[q], ep, peer).start()

    @phase
    def mix_home(q):
        both_g = pl.ds(2 * q, 2)
        wait_in(mix_all.at[pl.ds(0, n_tp - 1), both_g], mt_s, mt_r.at[q])
        mix_sum = mix_all[0, both_g]
        for k in range(1, n_tp):
            mix_sum = mix_sum + mix_all[k, both_g]
        mix_tot[both_g] = mix_sum
        for g in (2 * q, 2 * q + 1):
            for dx in range(NX):
                if g == home and dx == 0:
                    mix_in[ep] = mix_tot[home]
                else:
                    peer = ring(z, offsets[g], nz) * NX + ring(x, dx, NX)
                    rcopy(mix_tot.at[g], mix_in.at[ep], mx_s, mx_r, peer, tp).start()

    stage1(0)
    stage1(1)
    for k in range(3):
        poll(k)
    last = chunks - 1
    for q in range(last):
        ready(q)
        forward(q)
        poll(2 * q + 3)
        if q >= 1:
            rs_bc(q - 1)
        backward(q)
        element(q)
        poll(2 * q + 4)
        term(q)
        rs_a(q)
        if q >= 1:
            rs_de(q - 1)
        if q >= 2:
            rs_fg(q - 2)
        turn(q)
        mix_out(q)
        if q >= 1:
            mix_home(q - 1)

    ready(last)
    forward(last)
    rs_bc(last - 1)
    backward(last)
    element(last)
    turn(last)
    mix_out(last)
    term(last)
    rs_a(last)
    rs_de(last - 1)
    mix_home(last - 1)
    mix_home(last)
    rs_fg(last - 2)
    rs_bc(last)
    grads(0, 2)
    rs_fg(last - 1)
    grads(2, 3)
    rs_de(last)

    with jax.named_scope("mix_wait"):
        wait_in(mix_in.at[pl.ds(0, n_ep - 1)], mx_s, mx_r)
    for e in range(n_ep):
        mix_mat[e : e + 1, :] = mix_in[e]
    rank0, rank1, mix0, mix1, r0, r1 = (small[:, k : k + 1] for k in range(6))
    lane_f = (lanes - x * cap).astype(F32)

    def own_grad(route, rank):
        chosen = jnp.where(route == lane_e, 1.0, 0.0)
        spread = lax.dot_general(
            chosen, mix_mat[...], (((1,), (0,)), ((), ())),
            precision=lax.Precision.HIGHEST, preferred_element_type=F32,
        )
        return jnp.sum(jnp.where(rank == lane_f, spread, 0.0), axis=1, keepdims=True)

    grad0, grad1 = own_grad(r0, rank0), own_grad(r1, rank1)
    mixing_ref[0:1, :] = jnp.sum(jnp.where(diagonal, grad0, 0.0), axis=0, keepdims=True)
    mixing_ref[1:2, :] = jnp.sum(jnp.where(diagonal, grad1, 0.0), axis=0, keepdims=True)
    pairwise = mix0 * mix1
    route_grad = jnp.where(r0 == lanes_f, pairwise * (grad0 - grad1), 0.0)
    route_grad = route_grad + jnp.where(r1 == lanes_f, pairwise * (grad1 - grad0), 0.0)
    rg_hi, rg_lo = halves(route_grad)
    scale = 1.0 / math.sqrt(rows * n_ep)
    share = width // (n_ep * n_tp)
    per = cols // share
    turned_hi, turned_lo = rg_hi.T, rg_lo.T
    with jax.named_scope("router_part"):
        for k in range(n_tp):
            t = tok[:, k * cols : (k + 1) * cols]
            part = ((dot(turned_hi, t) + dot(turned_lo, t)) * scale).T.astype(BF16)
            rparts[k * per : (k + 1) * per] = part.reshape(per, share, 128)
    for _, pz, px in ep_peers:
        peer = pz * NX + px
        rcopy(rparts.at[peer * n_tp + tp], rin.at[ep], rt_s, rt_r, peer, tp).start()
    rin[ep] = rparts[ep * n_tp + tp]
    router_cols = router[:, pl.ds(pl.multiple_of(tp * cols, cols), cols)]
    path = dot(rg_hi[:, :experts], router_cols) + dot(rg_lo[:, :experts], router_cols)
    grads(3, 5)
    rs_fg(last)
    grads(5, n_tp)

    with jax.named_scope("ret_wait"):
        wait_in(ret_in.at[pl.ds(0, n_ep - 1)], ret_s, ret_r)
    token_part = dot(two_hot[...], ret_in[...].reshape(slots, cols))
    token_grad_ref[...] = (token_part + path).astype(BF16)
    with jax.named_scope("router_wait"):
        wait_in(rin.at[pl.ds(0, n_ep - 1)], rt_s, rt_r)
    acc = rin[0].astype(F32)
    for e in range(1, n_ep):
        acc = acc + rin[e].astype(F32)
    router_grad_ref[...] = acc[:, :experts]

    wait_out(ms_in.at[pl.ds(0, n_ep - 1)], ms_s, ms_r)
    wait_out(send.at[pl.ds(0, n_ep - 1)], a2a_s, a2a_r.at[0])
    wait_out(gathered.at[0], up_s, up_r.at[0])
    wait_out(gathered.at[0], dn_s, dn_r.at[0])
    wait_out(gathered.at[0, pl.ds(0, nz // 2)], two_up_s, two_r.at[0])
    wait_out(gathered.at[0, pl.ds(0, nz // 2)], two_dn_s, two_r.at[0])
    wait_out(gathered.at[pl.ds(0, NY)], pr_s, pr_r.at[0])
    wait_out(pair_in, ra_s, ra_r.at[0])
    wait_out(near_a, rb_s, rb_r.at[0])
    wait_out(near_b, rc_s, rc_r.at[0])
    wait_out(far_p, rd_s, rd_r.at[0])
    wait_out(far_m, re_s, re_r.at[0])
    wait_out(mix_all.at[pl.ds(0, n_tp - 1)], mt_s, mt_r)
    wait_out(mix_in.at[pl.ds(0, n_ep - 1)], mx_s, mx_r)
    wait_out(rin.at[pl.ds(0, n_ep - 1)], rt_s, rt_r)
    wait_out(ret_in.at[pl.ds(0, n_ep - 1)], ret_s, ret_r)


def hand_over(*refs):
    count = len(refs) // 2
    copies = [
        pltpu.make_async_copy(refs[k], refs[count + k], refs[-1].at[k]) for k in range(count)
    ]
    for copy in copies:
        copy.start()
    for copy in copies:
        copy.wait()


def solution(mesh):
    n_ep, n_tp = mesh.shape["ep"], mesh.shape["tp"]

    def local(tokens, routes, router_matrix, cotangent, gate_proj, up_proj, down_proj):
        rows, width = tokens.shape
        experts = router_matrix.shape[1]
        hidden = gate_proj.shape[2]
        hpad = -(-hidden // 128) * 128
        cap = rows * 2 * 2 // experts
        slots = experts * cap
        cols = width // n_tp
        nz = n_ep // NX
        group = NX * cap
        chunk, chunks = 2 * group, nz // 2
        share = width // (n_ep * n_tp)
        dma = pltpu.SemaphoreType.DMA
        vmem = pltpu.VMEM
        any_ = pl.BlockSpec(memory_space=pltpu.HBM)
        whole = pl.BlockSpec(memory_space=pltpu.VMEM)
        scratch = [
            vmem((rows, width), BF16), vmem((rows, cols), BF16), vmem((experts, width), BF16),
            vmem((2 * hpad, width), BF16), vmem((hpad, width), BF16),
            vmem((width, 2 * hpad), BF16), vmem((width, hpad), BF16),
            vmem((n_ep, cap, 2 * cols), BF16), vmem((slots // 128, 1, 128), F32),
            vmem((rows, slots), BF16), vmem((rows, 128), F32),
            vmem((n_tp, nz, group, 2 * cols), BF16), vmem((n_ep, 1, 128), F32),
            vmem((chunk, 2 * hpad), F32), vmem((chunk, hpad), F32),
            vmem((chunk, hpad), BF16), vmem((hpad, slots), BF16), vmem((slots, 2 * hpad), BF16),
            vmem((2 * hpad, slots), BF16),
            vmem((slots, 1), F32), vmem((chunk, 1), F32),
            vmem((2, NY, nz, group, cols), BF16), vmem((NY, nz, group, cols), BF16),
            vmem((chunks, group, cols), BF16), vmem((chunks, group, cols), BF16),
            vmem((nz, group, cols), BF16), vmem((nz, group, cols), BF16),
            vmem((nz, group, cols), BF16), vmem((n_ep, cap, cols), BF16),
            vmem((nz, 1, 128), F32), vmem((n_tp, nz, 1, 128), F32), vmem((nz, 1, 128), F32),
            vmem((n_ep, 1, 128), F32), vmem((n_ep, 128), F32),
            vmem((width // share, share, 128), BF16), vmem((n_ep, share, 128), BF16),
            dma((6,)),
            dma, dma, dma, dma((nz,)), dma, dma((nz,)), dma, dma((nz,)), dma, dma, dma((nz,)),
            dma, dma((nz,)),
            dma, dma((chunks,)), dma, dma((chunks,)), dma, dma((chunks,)), dma, dma((chunks,)),
            dma, dma((chunks,)),
            dma, dma((chunks,)), dma, dma, dma, dma, dma, dma,
        ]
        shape = jax.ShapeDtypeStruct
        results = pl.pallas_call(
            lambda *refs: kernel(n_ep, n_tp, hidden, *refs),
            out_shape=(
                shape((rows, cols), BF16), shape((2, rows), F32), shape((share, experts), F32),
                shape((hidden, width), BF16), shape((hidden, width), BF16),
                shape((hidden, width), BF16),
            ),
            in_specs=[any_, whole, any_, any_, any_, any_, any_],
            out_specs=(whole,) * 6,
            scratch_shapes=scratch,
            compiler_params=pltpu.CompilerParams(
                collective_id=0, has_side_effects=True, vmem_limit_bytes=VMEM_LIMIT
            ),
            name="moe_backward",
        )(
            *(
                pltpu.with_memory_space_constraint(a, pltpu.HBM)
                for a in (
                    tokens, routes.T, router_matrix.T, cotangent, jnp.swapaxes(gate_proj, 1, 2),
                    jnp.swapaxes(up_proj, 1, 2), down_proj,
                )
            )
        )
        token_grad, mixing, router_grad, gate_grad, up_grad, down_grad = pl.pallas_call(
            hand_over,
            out_shape=tuple(shape(r.shape, r.dtype) for r in results),
            in_specs=[whole] * 6,
            out_specs=(any_,) * 6,
            scratch_shapes=[dma((6,))],
            compiler_params=pltpu.CompilerParams(vmem_limit_bytes=2**20),
            name="hand_over",
        )(*results)
        return (
            token_grad, mixing.T, router_grad, gate_grad.T[None], up_grad.T[None], down_grad[None]
        )

    return jax.shard_map(
        local,
        mesh=mesh,
        in_specs=(
            P("ep", None), P("ep", None), P(), P("ep", "tp"),
            P("ep", None, "tp"), P("ep", None, "tp"), P("ep", "tp", None),
        ),
        out_specs=(
            P("ep", "tp"), P("ep", None), P(("ep", "tp"), None),
            P("ep", None, "tp"), P("ep", None, "tp"), P("ep", "tp", None),
        ),
        check_vma=False,
    )
```

```python
import math

import jax
import jax.numpy as jnp
from jax import lax
from jax.experimental import pallas as pl
from jax.experimental.pallas import tpu as pltpu
from jax.sharding import PartitionSpec as P

MESH = pl.DeviceIdType.MESH
BF16 = jnp.bfloat16
F32 = jnp.float32

NX, NY = 4, 4
OFFSETS = (0, 1, -2, 3, -3, 4, -1, 2)
VMEM_LIMIT = 47 * 2**20
OVER_ROWS = (((0,), (0,)), ((), ()))
OVER_COLS = (((1,), (1,)), ((), ()))


def dot(a, b, dims=None):
    if dims is None:
        return jnp.dot(a, b, preferred_element_type=F32)
    return lax.dot_general(a, b, dims, preferred_element_type=F32)


def iota(shape, dim):
    return lax.broadcasted_iota(jnp.int32, shape, dim)


def phase(step):
    def named(k):
        with jax.named_scope(step.__name__ + str(k)):
            return step(k)

    return named


def halves(value):
    high = value.astype(BF16)
    return high, (value - high.astype(F32)).astype(BF16)


def kernel(
    n_ep, n_tp, hidden,
    tokens_h, routes_ref, router_h, cot_h, gate_h, up_h, down_h,
    token_grad_ref, mixing_ref, router_grad_ref, gate_grad_ref, up_grad_ref, down_grad_ref,
    tok, cot, router, w2, wd, w2_t, wd_t,
    send, ms_send_buf, two_hot, small, gathered, ms_in,
    pre, back, hid, hid_t, gu, gu_t, ms_col, mix_col,
    terms, pair_in, near_a, near_b, far_p, far_m, total, ret_in,
    mix_row, mix_all, mix_tot, mix_in, mix_mat, rparts, rin,
    lsem,
    ms_s, ms_r, a2a_s, a2a_r, up_s, up_r, dn_s, dn_r, two_up_s, two_dn_s, two_r, pr_s, pr_r,
    ra_s, ra_r, rb_s, rb_r, rc_s, rc_r, rd_s, rd_r, re_s, re_r,
    mt_s, mt_r, mx_s, mx_r, rt_s, rt_r, ret_s, ret_r,
):
    nz = n_ep // NX
    rows, width = tok.shape
    experts = router.shape[0]
    cap = rows * 2 * 2 // experts
    cols = width // n_tp
    hpad = wd.shape[0]
    slots = experts * cap
    group = NX * cap
    chunk = 2 * group
    chunks = nz // 2
    ep, tp = lax.axis_index("ep"), lax.axis_index("tp")
    z, x = ep // NX, lax.rem(ep, NX)
    y, core = tp // 2, lax.rem(tp, 2)
    offsets = OFFSETS
    home = offsets.index(0)

    def ring(value, step, size):
        return lax.rem(value + (step + size), size)

    def tp_of(step):
        return ring(y, step, NY) * 2 + core

    tp_up, tp_dn, tp_far = tp_of(1), tp_of(-1), tp_of(2)
    partner = y * 2 + (1 - core)

    def rcopy(src, dst, s, r, e, t):
        return pltpu.make_async_remote_copy(
            src_ref=src, dst_ref=dst, send_sem=s, recv_sem=r, device_id=(e, t), device_id_type=MESH
        )

    def wait_in(ref, s, r):
        rcopy(ref, ref, s, r, ep, partner).wait_recv()

    def wait_out(ref, s, r):
        rcopy(ref, ref, s, r, ep, partner).wait_send()

    ep_peers = []
    for g, dz in enumerate(offsets):
        for dx in range(NX):
            if dz or dx:
                ep_peers.append((g, ring(z, -dz, nz), ring(x, dx, NX)))

    loads = [
        pltpu.make_async_copy(a, b, lsem.at[k])
        for k, (a, b) in enumerate(
            (
                (tokens_h, tok), (router_h, router), (cot_h, cot),
                (gate_h.at[0], w2.at[pl.ds(0, hidden)]),
                (up_h.at[0], w2.at[pl.ds(hpad, hidden)]),
                (down_h.at[0], wd.at[pl.ds(0, hidden)]),
            )
        )
    ]
    for load in loads:
        load.start()
    barrier = pltpu.get_barrier_semaphore()
    for _, pz, px in ep_peers:
        pl.semaphore_signal(barrier, inc=1, device_id=(pz * NX + px, tp), device_id_type=MESH)
    for d in range(1, n_tp):
        pl.semaphore_signal(barrier, inc=1, device_id=(ep, ring(tp, d, n_tp)), device_id_type=MESH)
    gap = jnp.zeros((hpad - hidden, width), BF16)
    w2[hidden:hpad, :] = gap
    w2[hpad + hidden :, :] = gap
    wd[hidden:, :] = gap
    with jax.named_scope("load"):
        loads[0].wait()
        loads[1].wait()

    lanes = iota((rows, 128), 1)
    diagonal = iota((rows, rows), 0) == iota((rows, rows), 1)

    def column(row):
        return jnp.sum(jnp.where(diagonal, row, 0.0), axis=1, keepdims=True)

    r0, r1 = (column(routes_ref[k : k + 1, :].astype(F32)) for k in range(2))
    lanes_f = lanes.astype(F32)
    oh0, oh1 = r0 == lanes_f, r1 == lanes_f
    both = jnp.where(oh0 | oh1, 1.0, 0.0).astype(BF16)
    before = jnp.where(iota((rows, rows), 0) > iota((rows, rows), 1), 1.0, 0.0).astype(BF16)
    earlier = dot(before, both)
    rank0 = jnp.sum(jnp.where(oh0, earlier, 0.0), axis=1, keepdims=True)
    rank1 = jnp.sum(jnp.where(oh1, earlier, 0.0), axis=1, keepdims=True)
    logits = dot(tok[...], router[...], OVER_COLS)
    lane_e = iota((rows, experts), 1).astype(F32)
    chosen0 = jnp.sum(jnp.where(r0 == lane_e, logits, 0.0), axis=1, keepdims=True)
    chosen1 = jnp.sum(jnp.where(r1 == lane_e, logits, 0.0), axis=1, keepdims=True)
    mix0 = jax.nn.sigmoid(chosen0 - chosen1)
    mix1 = jax.nn.sigmoid(chosen1 - chosen0)
    small[:, 0:1] = rank0
    small[:, 1:2] = rank1
    small[:, 2:3] = mix0
    small[:, 3:4] = mix1
    small[:, 4:5] = r0
    small[:, 5:6] = r1
    place0 = r0 * cap + rank0
    place1 = r1 * cap + rank1
    mb0 = mix0.astype(BF16).astype(F32)
    mb1 = mix1.astype(BF16).astype(F32)
    loads[2].wait()
    source = jnp.concatenate(
        [tok[:, pl.ds(pl.multiple_of(tp * cols, cols), cols)], cot[...]], axis=1
    )
    for k in range(slots // 128):
        at = (iota((rows, 128), 1) + k * 128).astype(F32)
        hit0, hit1 = place0 == at, place1 == at
        chosen = jnp.where(hit0 | hit1, 1.0, 0.0).astype(BF16)
        two_hot[:, k * 128 : (k + 1) * 128] = chosen
        ms_send_buf[k] = jnp.sum(
            jnp.where(hit0, mb0, 0.0) + jnp.where(hit1, mb1, 0.0), axis=0, keepdims=True
        )
        picked = dot(chosen, source, OVER_ROWS).astype(BF16)
        for m in range(128 // cap):
            send[k * (128 // cap) + m] = picked[m * cap : (m + 1) * cap]

    with jax.named_scope("barrier"):
        pl.semaphore_wait(barrier, len(ep_peers) + n_tp - 1)

    own_rows = pl.ds(pl.multiple_of(x * cap, cap), cap)
    for g, pz, px in ep_peers:
        peer, land = pz * NX + px, gathered.at[tp, g, own_rows]
        rcopy(ms_send_buf.at[pz], ms_in.at[g * NX + x], ms_s, ms_r, peer, tp).start()
        rcopy(send.at[peer], land, a2a_s, a2a_r.at[g], peer, tp).start()
    gathered[tp, home, own_rows, :] = send[ep]
    ms_in[home * NX + x] = ms_send_buf[z]
    with jax.named_scope("weights_in"):
        for load in loads[3:]:
            load.wait()

        def flip_weights(k, carry):
            at = pl.ds(pl.multiple_of(k * cols, cols), cols)
            w2_t[at, :] = w2[:, at].T
            wd_t[at, :] = wd[:, at].T
            return carry

        lax.fori_loop(0, n_tp, flip_weights, 0)

    def to_partner(share, g):
        piece = gathered.at[share, g]
        rcopy(piece, piece, pr_s, pr_r.at[g], ep, partner).start()

    @phase
    def stage1(g):
        if g == home:
            wait_in(gathered.at[tp, g, pl.ds(0, group - cap)], a2a_s, a2a_r.at[g])
        else:
            wait_in(gathered.at[tp, g], a2a_s, a2a_r.at[g])
        piece = gathered.at[tp, g]
        rcopy(piece, piece, up_s, up_r.at[g], ep, tp_up).start()
        rcopy(piece, piece, dn_s, dn_r.at[g], ep, tp_dn).start()
        to_partner(tp, g)

    @phase
    def stage2(g):
        below, above = gathered.at[tp_dn, g], gathered.at[tp_up, g]
        wait_in(below, up_s, up_r.at[g])
        if g % 2 == 0:
            rcopy(below, below, two_up_s, two_r.at[g], ep, tp_up).start()
        to_partner(tp_dn, g)
        wait_in(above, dn_s, dn_r.at[g])
        if g % 2 == 1:
            rcopy(above, above, two_dn_s, two_r.at[g], ep, tp_dn).start()
        to_partner(tp_up, g)

    @phase
    def stage3(g):
        wait_in(gathered.at[tp_far, g], two_up_s, two_r.at[g])
        to_partner(tp_far, g)

    @phase
    def stage4(g):
        wait_in(gathered.at[pl.ds(0, NY), g], pr_s, pr_r.at[g])

    def rows_of(q, lo):
        at = slice(2 * q, 2 * q + 2)
        return jnp.concatenate(
            [gathered[k, at, :, lo : lo + cols].reshape(chunk, cols) for k in range(n_tp)], axis=1
        )

    @phase
    def forward(q):
        pre[...] = dot(rows_of(q, 0), w2_t[...])

    @phase
    def backward(q):
        back[...] = dot(rows_of(q, cols), wd_t[...])
        if q == 0:
            wait_in(ms_in.at[pl.ds(0, n_ep - 1)], ms_s, ms_r)
        mine = iota((cap, 128), 1) == iota((cap, 128), 0) + x * cap
        spread = jnp.where(mine[None], ms_in[2 * q * NX : (2 * q + 2) * NX], 0.0)
        ms_col[pl.ds(q * chunk, chunk), :] = jnp.sum(spread, axis=2, keepdims=True).reshape(chunk, 1)

    @phase
    def element(q):
        def block_of(i, carry):
            block = pl.ds(pl.multiple_of(i * 32, 32), 32)
            out = pl.ds(pl.multiple_of(q * chunk + i * 32, 32), 32)
            a, u, b = pre[block, :hpad], pre[block, hpad:], back[block, :]
            sig = jax.nn.sigmoid(a)
            active = a * sig
            h = (active * u).astype(BF16)
            hid[block, :] = h
            mix_col[block, :] = jnp.sum(h.astype(F32) * b, axis=1, keepdims=True)
            scaled = ms_col[out, :] * b
            gu[out, :hpad] = (scaled * u * sig * (1.0 + a * (1.0 - sig))).astype(BF16)
            gu[out, hpad:] = (scaled * active).astype(BF16)
            return carry

        lax.fori_loop(0, chunk // 32, block_of, 0)

    @phase
    def term(q):
        def term_of(k, carry):
            w = w2[:, pl.ds(pl.multiple_of(k * 4 * cols, 4 * cols), 4 * cols)]
            t = dot(gu[pl.ds(q * chunk, chunk), :], w).astype(BF16)
            for m in range(4):
                piece = t[:, m * cols : (m + 1) * cols].reshape(2, group, cols)
                terms[m % 2, 2 * k + m // 2, 2 * q : 2 * q + 2] = piece
            return carry

        lax.fori_loop(0, n_tp // 4, term_of, 0)

    @phase
    def turn(q):
        eye = iota((group, group), 0) == iota((group, group), 1)
        for m in range(2):
            part = mix_col[m * group : (m + 1) * group, :]
            mix_row[2 * q + m] = jnp.sum(jnp.where(eye, part, 0.0), axis=0, keepdims=True)

    @phase
    def flip(q):
        hid_t[:, q * chunk : (q + 1) * chunk] = hid[...].T
        gu_t[:, q * chunk : (q + 1) * chunk] = gu[q * chunk : (q + 1) * chunk, :].T

    @phase
    def rs_a(q):
        both_g = pl.ds(2 * q, 2)
        rcopy(terms.at[1 - core, :, both_g], pair_in.at[:, both_g], ra_s, ra_r.at[q], ep, partner).start()

    def add_into(ref, index, other):
        ref[index] = (ref[index].astype(F32) + other.astype(F32)).astype(BF16)

    yu, yd, yf = ring(y, 1, NY), ring(y, -1, NY), ring(y, 2, NY)

    @phase
    def rs_bc(q):
        both_g = pl.ds(2 * q, 2)
        wait_in(pair_in.at[:, both_g], ra_s, ra_r.at[q])
        for k in (yf, yu, yd, y):
            for g in (2 * q, 2 * q + 1):
                add_into(terms, (core, k, g), pair_in[k, g])
        rcopy(terms.at[core, yf, 2 * q], near_a.at[q], rb_s, rb_r.at[q], ep, tp_up).start()
        rcopy(terms.at[core, yf, 2 * q + 1], near_b.at[q], rc_s, rc_r.at[q], ep, tp_dn).start()

    @phase
    def rs_de(q):
        both_g = pl.ds(2 * q, 2)
        wait_in(near_a.at[q], rb_s, rb_r.at[q])
        add_into(terms, (core, yu, 2 * q), near_a[q])
        rcopy(terms.at[core, yu, both_g], far_p.at[both_g], rd_s, rd_r.at[q], ep, tp_up).start()
        wait_in(near_b.at[q], rc_s, rc_r.at[q])
        add_into(terms, (core, yd, 2 * q + 1), near_b[q])
        rcopy(terms.at[core, yd, both_g], far_m.at[both_g], re_s, re_r.at[q], ep, tp_dn).start()

    @phase
    def rs_fg(q):
        both_g = pl.ds(2 * q, 2)
        wait_in(far_p.at[both_g], rd_s, rd_r.at[q])
        wait_in(far_m.at[both_g], re_s, re_r.at[q])
        for g in (2 * q, 2 * q + 1):
            summed = terms[core, y, g].astype(F32) + far_p[g].astype(F32) + far_m[g].astype(F32)
            total[g] = summed.astype(BF16)
            for dx in range(NX):
                if g == home and dx == 0:
                    continue
                pz, px = ring(z, offsets[g], nz), ring(x, dx, NX)
                piece = total.at[g, pl.ds(pl.multiple_of(px * cap, cap), cap)]
                rcopy(piece, ret_in.at[ep], ret_s, ret_r, pz * NX + px, tp).start()
        if q == home // 2:
            ret_in[ep] = total[home, own_rows, :]

    def weights(k, carry):
        def all_rows(lo):
            return gathered[k, :, :, lo : lo + cols].reshape(slots, cols)

        at = pl.ds(pl.multiple_of(k * cols, cols), cols)
        both_grads = dot(gu_t[...], all_rows(0)).astype(BF16)
        gate_grad_ref[:, at] = both_grads[:hidden]
        up_grad_ref[:, at] = both_grads[hpad : hpad + hidden]
        scaled = (ms_col[...] * all_rows(cols).astype(F32)).astype(BF16)
        down_grad_ref[:, at] = dot(hid_t[...], scaled)[:hidden].astype(BF16)
        return carry

    def poll(k):
        if k < nz:
            stage2(k)
        if k + 2 < nz:
            stage1(k + 2)
        if k:
            stage3(k - 1)

    def ready(q):
        stage4(2 * q)
        stage4(2 * q + 1)

    def grads(lo, hi):
        with jax.named_scope("grads" + str(lo)):
            lax.fori_loop(lo, hi, weights, 0)

    def mix_out(q):
        both_g = pl.ds(2 * q, 2)
        mix_all[tp, both_g] = mix_row[both_g]
        for d in range(1, n_tp):
            peer = ring(tp, d, n_tp)
            rcopy(mix_row.at[both_g], mix_all.at[tp, both_g], mt_s, mt_r.at[q], ep, peer).start()

    @phase
    def mix_home(q):
        both_g = pl.ds(2 * q, 2)
        wait_in(mix_all.at[pl.ds(0, n_tp - 1), both_g], mt_s, mt_r.at[q])
        mix_sum = mix_all[0, both_g]
        for k in range(1, n_tp):
            mix_sum = mix_sum + mix_all[k, both_g]
        mix_tot[both_g] = mix_sum
        for g in (2 * q, 2 * q + 1):
            for dx in range(NX):
                if g == home and dx == 0:
                    mix_in[ep] = mix_tot[home]
                else:
                    peer = ring(z, offsets[g], nz) * NX + ring(x, dx, NX)
                    rcopy(mix_tot.at[g], mix_in.at[ep], mx_s, mx_r, peer, tp).start()

    stage1(0)
    stage1(1)
    for k in range(3):
        poll(k)
    last = chunks - 1
    for q in range(last):
        ready(q)
        forward(q)
        poll(2 * q + 3)
        if q >= 1:
            rs_bc(q - 1)
        backward(q)
        element(q)
        if q < last - 1:
            poll(2 * q + 4)
        term(q)
        rs_a(q)
        if q == last - 1:
            poll(2 * q + 4)
        turn(q)
        mix_out(q)
        flip(q)
        if q >= 1:
            mix_home(q - 1)
            rs_de(q - 1)
        if q >= 2:
            rs_fg(q - 2)

    ready(last)
    forward(last)
    rs_bc(last - 1)
    backward(last)
    element(last)
    turn(last)
    mix_out(last)
    term(last)
    rs_a(last)
    flip(last)
    rs_de(last - 1)
    rs_bc(last)
    rs_fg(last - 2)
    mix_home(last - 1)
    grads(0, 3)
    mix_home(last)
    grads(3, 5)
    rs_fg(last - 1)
    rs_de(last)
    grads(5, 6)

    with jax.named_scope("mix_wait"):
        wait_in(mix_in.at[pl.ds(0, n_ep - 1)], mx_s, mx_r)
    for e in range(n_ep):
        mix_mat[e : e + 1, :] = mix_in[e]
    rank0, rank1, mix0, mix1, r0, r1 = (small[:, k : k + 1] for k in range(6))
    lane_f = (lanes - x * cap).astype(F32)

    def own_grad(route, rank):
        chosen = jnp.where(route == lane_e, 1.0, 0.0)
        spread = lax.dot_general(
            chosen, mix_mat[...], (((1,), (0,)), ((), ())),
            precision=lax.Precision.HIGHEST, preferred_element_type=F32,
        )
        return jnp.sum(jnp.where(rank == lane_f, spread, 0.0), axis=1, keepdims=True)

    grad0, grad1 = own_grad(r0, rank0), own_grad(r1, rank1)
    mixing_ref[0:1, :] = jnp.sum(jnp.where(diagonal, grad0, 0.0), axis=0, keepdims=True)
    mixing_ref[1:2, :] = jnp.sum(jnp.where(diagonal, grad1, 0.0), axis=0, keepdims=True)
    pairwise = mix0 * mix1
    route_grad = jnp.where(r0 == lanes_f, pairwise * (grad0 - grad1), 0.0)
    route_grad = route_grad + jnp.where(r1 == lanes_f, pairwise * (grad1 - grad0), 0.0)
    rg_hi, rg_lo = halves(route_grad)
    scale = 1.0 / math.sqrt(rows * n_ep)
    share = width // (n_ep * n_tp)
    per = cols // share
    turned_hi, turned_lo = rg_hi.T, rg_lo.T
    with jax.named_scope("router_part"):
        for k in range(n_tp):
            t = tok[:, k * cols : (k + 1) * cols]
            part = ((dot(turned_hi, t) + dot(turned_lo, t)) * scale).T.astype(BF16)
            rparts[k * per : (k + 1) * per] = part.reshape(per, share, 128)
    for _, pz, px in ep_peers:
        peer = pz * NX + px
        rcopy(rparts.at[peer * n_tp + tp], rin.at[ep], rt_s, rt_r, peer, tp).start()
    rin[ep] = rparts[ep * n_tp + tp]
    router_cols = router[:, pl.ds(pl.multiple_of(tp * cols, cols), cols)]
    path = dot(rg_hi[:, :experts], router_cols) + dot(rg_lo[:, :experts], router_cols)
    rs_fg(last)
    grads(6, n_tp)

    with jax.named_scope("ret_wait"):
        wait_in(ret_in.at[pl.ds(0, n_ep - 1)], ret_s, ret_r)
    token_part = dot(two_hot[...], ret_in[...].reshape(slots, cols))
    token_grad_ref[...] = (token_part + path).astype(BF16)
    with jax.named_scope("router_wait"):
        wait_in(rin.at[pl.ds(0, n_ep - 1)], rt_s, rt_r)
    acc = rin[0].astype(F32)
    for e in range(1, n_ep):
        acc = acc + rin[e].astype(F32)
    router_grad_ref[...] = acc[:, :experts]

    wait_out(ms_in.at[pl.ds(0, n_ep - 1)], ms_s, ms_r)
    wait_out(send.at[pl.ds(0, n_ep - 1)], a2a_s, a2a_r.at[0])
    wait_out(gathered.at[0], up_s, up_r.at[0])
    wait_out(gathered.at[0], dn_s, dn_r.at[0])
    wait_out(gathered.at[0, pl.ds(0, nz // 2)], two_up_s, two_r.at[0])
    wait_out(gathered.at[0, pl.ds(0, nz // 2)], two_dn_s, two_r.at[0])
    wait_out(gathered.at[pl.ds(0, NY)], pr_s, pr_r.at[0])
    wait_out(pair_in, ra_s, ra_r.at[0])
    wait_out(near_a, rb_s, rb_r.at[0])
    wait_out(near_b, rc_s, rc_r.at[0])
    wait_out(far_p, rd_s, rd_r.at[0])
    wait_out(far_m, re_s, re_r.at[0])
    wait_out(mix_all.at[pl.ds(0, n_tp - 1)], mt_s, mt_r)
    wait_out(mix_in.at[pl.ds(0, n_ep - 1)], mx_s, mx_r)
    wait_out(rin.at[pl.ds(0, n_ep - 1)], rt_s, rt_r)
    wait_out(ret_in.at[pl.ds(0, n_ep - 1)], ret_s, ret_r)


def hand_over(*refs):
    count = len(refs) // 2
    copies = [
        pltpu.make_async_copy(refs[k], refs[count + k], refs[-1].at[k]) for k in range(count)
    ]
    for copy in copies:
        copy.start()
    for copy in copies:
        copy.wait()


def solution(mesh):
    n_ep, n_tp = mesh.shape["ep"], mesh.shape["tp"]

    def local(tokens, routes, router_matrix, cotangent, gate_proj, up_proj, down_proj):
        rows, width = tokens.shape
        experts = router_matrix.shape[1]
        hidden = gate_proj.shape[2]
        hpad = -(-hidden // 128) * 128
        cap = rows * 2 * 2 // experts
        slots = experts * cap
        cols = width // n_tp
        nz = n_ep // NX
        group = NX * cap
        chunk, chunks = 2 * group, nz // 2
        share = width // (n_ep * n_tp)
        dma = pltpu.SemaphoreType.DMA
        vmem = pltpu.VMEM
        any_ = pl.BlockSpec(memory_space=pltpu.HBM)
        whole = pl.BlockSpec(memory_space=pltpu.VMEM)
        scratch = [
            vmem((rows, width), BF16), vmem((rows, cols), BF16), vmem((experts, width), BF16),
            vmem((2 * hpad, width), BF16), vmem((hpad, width), BF16),
            vmem((width, 2 * hpad), BF16), vmem((width, hpad), BF16),
            vmem((n_ep, cap, 2 * cols), BF16), vmem((slots // 128, 1, 128), F32),
            vmem((rows, slots), BF16), vmem((rows, 128), F32),
            vmem((n_tp, nz, group, 2 * cols), BF16), vmem((n_ep, 1, 128), F32),
            vmem((chunk, 2 * hpad), F32), vmem((chunk, hpad), F32),
            vmem((chunk, hpad), BF16), vmem((hpad, slots), BF16), vmem((slots, 2 * hpad), BF16),
            vmem((2 * hpad, slots), BF16),
            vmem((slots, 1), F32), vmem((chunk, 1), F32),
            vmem((2, NY, nz, group, cols), BF16), vmem((NY, nz, group, cols), BF16),
            vmem((chunks, group, cols), BF16), vmem((chunks, group, cols), BF16),
            vmem((nz, group, cols), BF16), vmem((nz, group, cols), BF16),
            vmem((nz, group, cols), BF16), vmem((n_ep, cap, cols), BF16),
            vmem((nz, 1, 128), F32), vmem((n_tp, nz, 1, 128), F32), vmem((nz, 1, 128), F32),
            vmem((n_ep, 1, 128), F32), vmem((n_ep, 128), F32),
            vmem((width // share, share, 128), BF16), vmem((n_ep, share, 128), BF16),
            dma((6,)),
            dma, dma, dma, dma((nz,)), dma, dma((nz,)), dma, dma((nz,)), dma, dma, dma((nz,)),
            dma, dma((nz,)),
            dma, dma((chunks,)), dma, dma((chunks,)), dma, dma((chunks,)), dma, dma((chunks,)),
            dma, dma((chunks,)),
            dma, dma((chunks,)), dma, dma, dma, dma, dma, dma,
        ]
        shape = jax.ShapeDtypeStruct
        results = pl.pallas_call(
            lambda *refs: kernel(n_ep, n_tp, hidden, *refs),
            out_shape=(
                shape((rows, cols), BF16), shape((2, rows), F32), shape((share, experts), F32),
                shape((hidden, width), BF16), shape((hidden, width), BF16),
                shape((hidden, width), BF16),
            ),
            in_specs=[any_, whole, any_, any_, any_, any_, any_],
            out_specs=(whole,) * 6,
            scratch_shapes=scratch,
            compiler_params=pltpu.CompilerParams(
                collective_id=0, has_side_effects=True, vmem_limit_bytes=VMEM_LIMIT
            ),
            name="moe_backward",
        )(
            *(
                pltpu.with_memory_space_constraint(a, pltpu.HBM)
                for a in (
                    tokens, routes.T, router_matrix.T, cotangent, jnp.swapaxes(gate_proj, 1, 2),
                    jnp.swapaxes(up_proj, 1, 2), down_proj,
                )
            )
        )
        token_grad, mixing, router_grad, gate_grad, up_grad, down_grad = pl.pallas_call(
            hand_over,
            out_shape=tuple(shape(r.shape, r.dtype) for r in results),
            in_specs=[whole] * 6,
            out_specs=(any_,) * 6,
            scratch_shapes=[dma((6,))],
            compiler_params=pltpu.CompilerParams(vmem_limit_bytes=2**20),
            name="hand_over",
        )(*results)
        return (
            token_grad, mixing.T, router_grad, gate_grad.T[None], up_grad.T[None], down_grad[None]
        )

    return jax.shard_map(
        local,
        mesh=mesh,
        in_specs=(
            P("ep", None), P("ep", None), P(), P("ep", "tp"),
            P("ep", None, "tp"), P("ep", None, "tp"), P("ep", "tp", None),
        ),
        out_specs=(
            P("ep", "tp"), P("ep", None), P(("ep", "tp"), None),
            P("ep", None, "tp"), P("ep", None, "tp"), P("ep", "tp", None),
        ),
        check_vma=False,
    )
```
